32 devices in a mesh: sp: 8 (over z, y), tp: 4 (over x, core).
Axes of the slice: x: 2, y: 2, z: 4, core: 2. Of those that a mesh axis runs over, the one named last changes fastest.
Arguments:
- queries: bfloat16 [4096, 512], P('sp', 'tp'), may hold values from -6 to 6
- keys: bfloat16 [4096, 512], P('sp', 'tp'), may hold values from -6 to 6
- values: bfloat16 [4096, 1024], P('sp', 'tp'), may hold values from -6 to 6
- input_gate_log: float32 [8, 4096], P('tp', 'sp'), may hold values from -5 to 128
- forget_gate_logits: float32 [8, 4096], P('tp', 'sp'), may hold values from 1 to 16
- extra_decay_log: float32 [8, 4096], P('tp', 'sp'), may hold values from -1 to 0
- output_gate_logits: bfloat16 [4096, 1024], P('sp', 'tp'), may hold values from -6 to 6
- head_norm_scale: float32 [1024], P('tp'), may hold values from 0.1 to 1.9
- layer_residual_input: bfloat16 [4096, 2048], P(('sp', 'tp')), may hold values from -6 to 6
- output_projection_weight: bfloat16 [1024, 2048], replicated, may hold values from -0.1875 to 0.1875
- expert_norm_scale: float32 [2048], replicated, may hold values from 0.1 to 1.9
- routing_expert_index: int32 [4096, 2], P(('sp', 'tp')), may hold values from 0 to 31, all different within a row; in each aligned block of 128 rows (0 to 127, 128 to 255, ...) at most 16 rows name the same one
- routing_expert_weight: float32 [4096, 2], P(('sp', 'tp')), may hold values from 0.2 to 1
- expert_gate_weight: bfloat16 [32, 2048, 1024], P(('sp', 'tp')), may hold values from -0.125 to 0.125
- expert_up_weight: bfloat16 [32, 2048, 1024], P(('sp', 'tp')), may hold values from -0.125 to 0.125
- expert_down_weight: bfloat16 [32, 1024, 2048], P(('sp', 'tp')), may hold values from -0.1875 to 0.1875
Outputs:
- result: bfloat16 [4096, 2048], P(('sp', 'tp'))
The draws below stay inside these ranges and needn't reach their ends.
Inputs may be any that keep to these rules, and one draw needn't show every extreme that they name: `routing_expert_index`: each row names 2 different experts. Within each aligned block of 128 rows (the rows of one device) no expert is named more than 16 times, a bound that some block reaches in every draw.
All inputs are finite; a program needn't handle non-finite values.
Results may differ from the reference program's by a relative error of at most 0.013.
Values may be sent and summed in bfloat16 or wider, within the bound.
A program may use at most 64 MiB of HBM per device.

```python
import math
import jax
import jax.numpy as jnp
import numpy as np
from jax import lax

D = 2048
HEADS = 8
DQK = 64
DV = 128
FF = 1024
TOP = 2
BLOCK = 128
TOK_DEV = 512
TOKENS = 4096
ROWS = 128
EXPERTS = 32
CAP = 16
N_SP = 8
N_TP = 4


def draw_input_gate_log(key, part):
    gate_values = jax.random.truncated_normal(jax.random.fold_in(key, 21), -5.0, 5.0, (HEADS, TOKENS), jnp.float32)
    return gate_values


def draw_forget_gate_logits(key, part):
    order_key, fast_key, jitter_key, shift_key = jax.random.split(jax.random.fold_in(key, 31), 4)
    head_order = jax.random.permutation(order_key, HEADS)
    slow_count = HEADS // 2
    is_slow = (head_order < slow_count)[:, None]
    fast_level = jax.random.uniform(fast_key, (HEADS, 1), jnp.float32, 3.5, 4.5)
    slow_level = jnp.log(jnp.float32(TOKENS)) + 1.5
    jitter = 0.7 * jax.random.truncated_normal(jitter_key, -2.0, 2.0, (HEADS, TOKENS), jnp.float32)
    device_shift = jax.random.uniform(shift_key, (HEADS, TOKENS // TOK_DEV, 1), jnp.float32, -0.35, 0.35)
    device_shift = jnp.broadcast_to(device_shift, (HEADS, TOKENS // TOK_DEV, TOK_DEV)).reshape(HEADS, TOKENS)
    return jnp.where(is_slow, slow_level, fast_level) + jitter + device_shift


def draw_extra_decay_log(key, part):
    spot_key, loss_key = jax.random.split(jax.random.fold_in(key, 41), 2)
    spot_index = jax.random.randint(spot_key, (HEADS, 3), 0, TOKENS)
    losses = jax.random.uniform(loss_key, (HEADS, 3), jnp.float32, -0.6931, -0.2231)
    head_rows = jnp.broadcast_to(jnp.arange(HEADS)[:, None], (HEADS, 3))
    return jnp.zeros((HEADS, TOKENS), jnp.float32).at[head_rows, spot_index].set(losses)


def levels(own_key, dims, cuts, least, high):
    loudness, own = 1.0, jax.random.fold_in(own_key, 6)
    for dim, blocks in cuts:
        heights = jnp.exp(jax.random.uniform(jax.random.fold_in(own, dim), (blocks,), jnp.float32, least / len(cuts), high / len(cuts)))
        loudness = loudness * jnp.repeat(heights, dims[dim] // blocks).reshape([-1 if axis == dim else 1 for axis in range(len(dims))])
    return loudness


def shared_out(rng, own, number, rows, number_of, top, reach, slope):
    order = jax.random.permutation(rng, number_of)
    crowded, common = shares(number_of, rows * top, reach, slope, True), shares(number_of, rows * top, reach, slope, False)
    places = jnp.arange(number_of)

    def named(sizes, rotation):
        used = int((sizes > 0).sum())
        fixed = max(1, used // 4)
        moved = fixed + (places - fixed + rotation * (used - fixed)) % max(1, number_of - fixed)
        return jnp.zeros((number_of,), jnp.int32).at[order[jnp.where(places < fixed, places, moved)]].set(jnp.asarray(sizes, jnp.int32))

    sizes = jnp.where(number % 4 == 0, named(crowded, number // 4), named(common, number - number // 4 - 1))
    mixed = jax.random.permutation(jax.random.fold_in(own, 3), number_of)
    giver, taker = mixed[0:number_of // 2 * 2:2], mixed[1:number_of // 2 * 2:2]
    slack = jnp.minimum(sizes[giver] - 1, reach - sizes[taker]) // 2
    slack = jnp.where((giver == order[0]) | (taker == order[0]) | (sizes[taker] == 0), 0, jnp.maximum(slack, 0))
    moved = jax.random.randint(jax.random.fold_in(own, 4), (number_of // 2,), 0, 1 << 20) % (slack + 1)
    sizes = sizes.at[giver].add(-moved).at[taker].add(moved)
    members = jnp.searchsorted(jnp.cumsum(sizes), jnp.arange(rows * top), side="right").astype(jnp.int32)
    listing = members.reshape(top, rows).T
    listing = listing[jax.random.permutation(jax.random.fold_in(own, 1), rows)]
    rotation = jax.random.randint(jax.random.fold_in(own, 2), (rows, 1), 0, top)
    return jnp.take_along_axis(listing, (jnp.arange(top)[None, :] + rotation) % top, axis=1)


def shares(count, total, limit, lean, full):
    loads = [(1 << 20) // math.isqrt(grade ** lean) + 1 for grade in range(1, count + 1)]
    largest = limit if full else min(limit, max(-(-total // count), total * loads[0] // sum(loads)))
    least = 1 if total - largest >= count - 1 else 0
    holding, spare = [largest] + [least] * (count - 1), total - largest - least * (count - 1)
    while spare > 0:
        movable = [i for i in range(1, count) if holding[i] < largest] or [i for i in range(1, count) if holding[i] < limit]
        mass, remaining = sum([loads[i] for i in movable]), spare
        for i in movable:
            extra = min(limit - holding[i], max(1, remaining * loads[i] // mass), spare)
            holding[i] = holding[i] + extra
            spare = spare - extra
    return np.array(holding)


def normal_values(stream_key, extent, width, limit, cuts=(), kind=jnp.bfloat16):
    array = width * jax.random.normal(stream_key, extent, jnp.float32)
    if cuts:
        array = array * levels(stream_key, extent, cuts, -0.22, 0.18)
    return jnp.clip(array, -limit, limit).astype(kind)


def setup_inputs(seed: int = 0) -> dict:
    seeds = jax.random.split(jax.random.key(seed), 17)
    queries = normal_values(seeds[0], (TOKENS, HEADS * DQK), 1.0, 6.0, ((0, 8), (1, 4)))
    keys = normal_values(seeds[1], (TOKENS, HEADS * DQK), 1.0, 6.0, ((0, 8), (1, 4)))
    values = normal_values(seeds[2], (TOKENS, HEADS * DV), 1.0, 6.0, ((0, 8), (1, 4)))
    input_gate_log = draw_input_gate_log(jax.random.fold_in(seeds[16], 71), 0)
    forget_gate_logits = draw_forget_gate_logits(jax.random.fold_in(seeds[16], 71), 0)
    extra_decay_log = draw_extra_decay_log(jax.random.fold_in(seeds[16], 71), 0)
    output_gate_logits = normal_values(seeds[6], (TOKENS, HEADS * DV), 1.0, 6.0, ((0, 8), (1, 4)))
    head_norm_scale = jnp.clip(1.0 + 0.18 * jax.random.normal(seeds[7], (HEADS * DV,), jnp.float32), 0.1, 1.9)
    layer_residual_input = normal_values(seeds[8], (TOKENS, D), 1.0, 6.0, ((0, 32),))
    output_projection_weight = normal_values(seeds[9], (HEADS * DV, D), (HEADS * DV) ** -0.5, 0.1875)
    expert_norm_scale = jnp.clip(1.0 + 0.18 * jax.random.normal(seeds[10], (D,), jnp.float32), 0.1, 1.9)
    routing_expert_index_keys = jax.random.split(jax.random.fold_in(seeds[11], 1), TOKENS // ROWS)
    routing_expert_index_turns = jax.random.permutation(jax.random.fold_in(seeds[11], 3), TOKENS // ROWS)
    routing_expert_index = jax.vmap(lambda own, number: shared_out(jax.random.fold_in(seeds[11], 2), own, number, ROWS, EXPERTS, TOP, CAP, 1))(routing_expert_index_keys, routing_expert_index_turns).reshape((TOKENS, TOP))
    routing_expert_weight = jnp.clip(0.2 + 0.8 * jax.random.uniform(seeds[12], (TOKENS, TOP), jnp.float32) ** levels(seeds[12], (TOKENS, TOP), ((0, 32),), -0.2, 0.2), 0.2, 1.0)
    expert_gate_weight = normal_values(seeds[13], (EXPERTS, D, FF), D ** -0.5, 0.125, ((0, 32),))
    expert_up_weight = normal_values(seeds[14], (EXPERTS, D, FF), D ** -0.5, 0.125, ((0, 32),))
    expert_down_weight = normal_values(seeds[15], (EXPERTS, FF, D), FF ** -0.5, 0.1875, ((0, 32),))
    return dict(queries=queries, keys=keys, values=values, input_gate_log=input_gate_log, forget_gate_logits=forget_gate_logits, extra_decay_log=extra_decay_log, output_gate_logits=output_gate_logits, head_norm_scale=head_norm_scale, layer_residual_input=layer_residual_input, output_projection_weight=output_projection_weight, expert_norm_scale=expert_norm_scale, routing_expert_index=routing_expert_index, routing_expert_weight=routing_expert_weight, expert_gate_weight=expert_gate_weight, expert_up_weight=expert_up_weight, expert_down_weight=expert_down_weight)


very_low = -1e+30
epsilon = 1e-06
highest = lax.Precision.HIGHEST

def block_step(carried, inputs):
    memory, stabilizer = carried
    query_blk, key_blk, value_blk, input_blk, forget_blk = inputs
    length = query_blk.shape[1]
    within = jnp.cumsum(forget_blk, axis=-1)
    causal = jnp.arange(length)[:, None] >= jnp.arange(length)[None, :]
    log_weight = jnp.where(causal, within[:, :, None] - within[:, None, :] + input_blk[:, None, :], very_low)
    from_state = within + stabilizer[:, None]
    largest = jnp.maximum(from_state, lax.optimization_barrier(jnp.max(log_weight, axis=-1)))
    intra_weight = jnp.exp(log_weight - largest[:, :, None])
    state_weight = jnp.exp(from_state - largest)
    scores = jnp.einsum('htd,hsd->hts', query_blk, key_blk, precision=highest) * intra_weight
    numerator = jnp.einsum('hts,hsv->htv', scores, value_blk, precision=highest) + state_weight[:, :, None] * jnp.einsum('htd,hdv->htv', query_blk, memory, precision=highest)
    block_total = within[:, -1]
    to_end = block_total[:, None] - within + input_blk
    new_stabilizer = jnp.maximum(block_total + stabilizer, lax.optimization_barrier(jnp.max(to_end, axis=-1)))
    retain = jnp.exp(block_total + stabilizer - new_stabilizer)
    state_add = jnp.exp(to_end - new_stabilizer[:, None])
    memory = retain[:, None, None] * memory + jnp.einsum('hsd,hsv->hdv', key_blk * state_add[:, :, None], value_blk, precision=highest)
    return ((memory, new_stabilizer), numerator)

def reference(queries, keys, values, input_gate_log, forget_gate_logits, extra_decay_log, output_gate_logits, head_norm_scale, layer_residual_input, output_projection_weight, expert_norm_scale, routing_expert_index, routing_expert_weight, expert_gate_weight, expert_up_weight, expert_down_weight):
    blocks = TOKENS // BLOCK

    def to_blocks(matrix, columns):
        return matrix.astype(jnp.float32).reshape(blocks, BLOCK, HEADS, columns).transpose(0, 2, 1, 3)

    def gate_blocks(matrix):
        return matrix.reshape(HEADS, blocks, BLOCK).transpose(1, 0, 2)
    query_blocks = to_blocks(queries, DQK) * DQK ** (-0.5)
    key_blocks = to_blocks(keys, DQK)
    value_blocks = to_blocks(values, DV)
    forget_log_value = jax.nn.log_sigmoid(forget_gate_logits) + extra_decay_log
    initial = (jnp.zeros((HEADS, DQK, DV), jnp.float32), jnp.zeros((HEADS,), jnp.float32))
    unused, numerator = lax.scan(block_step, initial, (query_blocks, key_blocks, value_blocks, gate_blocks(input_gate_log), gate_blocks(forget_log_value)))
    cell_out = numerator.transpose(0, 2, 1, 3).reshape(TOKENS, HEADS, DV)
    scaled = cell_out * lax.rsqrt(lax.optimization_barrier(jnp.mean(cell_out * cell_out, axis=-1, keepdims=True)) + epsilon)
    gated_out = jax.nn.sigmoid(output_gate_logits.astype(jnp.float32)).reshape(TOKENS, HEADS, DV) * scaled * head_norm_scale.reshape(HEADS, DV)
    mixture = gated_out.reshape(TOKENS, HEADS * DV).astype(jnp.bfloat16)
    middle = (layer_residual_input.astype(jnp.float32) + jnp.dot(mixture, output_projection_weight, preferred_element_type=jnp.float32)).astype(jnp.bfloat16)
    middle_wide = middle.astype(jnp.float32)
    normed = (middle_wide * lax.rsqrt(lax.optimization_barrier(jnp.mean(middle_wide * middle_wide, axis=-1, keepdims=True)) + epsilon) * expert_norm_scale).astype(jnp.bfloat16)
    flat_ids = routing_expert_index.reshape(-1)
    flat_weights = routing_expert_weight.reshape(-1)
    most_rows = CAP * N_SP * N_TP

    def one_expert(expert_id, running):
        chosen = flat_ids == expert_id
        picked = jnp.nonzero(chosen, size=most_rows, fill_value=0)[0].astype(jnp.int32)
        in_range = jnp.arange(most_rows) < jnp.sum(chosen)
        token_rows = picked // TOP
        expert_rows = jnp.take(normed, token_rows, axis=0)
        gate_part = jnp.dot(expert_rows, expert_gate_weight[expert_id], preferred_element_type=jnp.float32)
        up_part = jnp.dot(expert_rows, expert_up_weight[expert_id], preferred_element_type=jnp.float32)
        activation = (jax.nn.silu(gate_part) * up_part).astype(jnp.bfloat16)
        produced = jnp.dot(activation, expert_down_weight[expert_id], preferred_element_type=jnp.float32).astype(jnp.bfloat16)
        row_weight = jnp.where(in_range, jnp.take(flat_weights, picked), jnp.float32(0.0))
        return running.at[token_rows].add(row_weight[:, None] * produced.astype(jnp.float32))
    expert_sum = lax.fori_loop(0, EXPERTS, one_expert, jnp.zeros((TOKENS, D), jnp.float32))
    return (middle_wide + expert_sum).astype(jnp.bfloat16)
```

```python
import functools

import jax
import jax.numpy as jnp
from jax import lax
from jax.experimental import pallas as pl
from jax.experimental.pallas import tpu as pltpu
from jax.sharding import PartitionSpec as P

TOP = 2
BLOCK = 128


very_low = -1e30
epsilon = 1e-06
highest = lax.Precision.HIGHEST
MESH = pl.DeviceIdType.MESH


def join_kernel(n, heads, key_width, memory_ref, scalars_ref, out_memory, out_scalars,
                got_memory, got_scalars, send_memory, send_scalars, recv_memory, recv_scalars):
    me = lax.axis_index("sp")
    barrier = pltpu.get_barrier_semaphore()
    for k in range(1, n):
        other = lax.rem(me + k, n)
        pl.semaphore_signal(barrier, inc=1, device_id={"sp": other}, device_id_type=MESH)
    pl.semaphore_wait(barrier, n - 1)

    def copies(source, target):
        kind = dict(device_id={"sp": target}, device_id_type=MESH)
        return (
            pltpu.make_async_remote_copy(
                src_ref=memory_ref, dst_ref=got_memory.at[source],
                send_sem=send_memory.at[target], recv_sem=recv_memory.at[source], **kind),
            pltpu.make_async_remote_copy(
                src_ref=scalars_ref, dst_ref=got_scalars.at[source],
                send_sem=send_scalars.at[target], recv_sem=recv_scalars.at[source], **kind),
        )

    for k in range(n - 1, 0, -1):
        @pl.when(me + k < n)
        def _(k=k):
            for copy in copies(me, me + k):
                copy.start()

    out_memory[...] = jnp.zeros_like(out_memory)
    out_scalars[...] = jnp.full_like(out_scalars, very_low)

    def lap(j, carry):
        for copy in copies(j, me):
            copy.wait_recv()
        for h in range(heads):
            decay = got_scalars[j, h : h + 1, :]
            stab_late = got_scalars[j, heads + h : heads + h + 1, :]
            shifted = decay + out_scalars[h : h + 1, :]
            combined = jnp.maximum(shifted, stab_late)
            rows = slice(h * key_width, (h + 1) * key_width)
            out_memory[rows, :] = jnp.exp(shifted - combined) * out_memory[rows, :] + jnp.exp(
                stab_late - combined
            ) * got_memory[j, rows, :].astype(jnp.float32)
            out_scalars[h : h + 1, :] = combined
        return carry

    lax.fori_loop(0, me, lap, 0)
    for k in range(1, n):
        @pl.when(me + k < n)
        def _(k=k):
            for copy in copies(me, me + k):
                copy.wait_send()


def incoming_state(decay, memory, stabilizer):
    heads, key_width, value_width = memory.shape
    n = lax.axis_size("sp")
    scalar_rows = -(-2 * heads // 8) * 8
    scalars = jnp.concatenate(
        [decay, stabilizer, jnp.zeros((scalar_rows - 2 * heads,), jnp.float32)]
    )
    scalars = jnp.broadcast_to(scalars[:, None], (scalar_rows, value_width))
    flat = memory.reshape(heads * key_width, value_width).astype(jnp.bfloat16)
    vmem = pl.BlockSpec(memory_space=pltpu.VMEM)
    out_memory, out_scalars = pl.pallas_call(
        functools.partial(join_kernel, n, heads, key_width),
        out_shape=(
            jax.ShapeDtypeStruct(flat.shape, jnp.float32),
            jax.ShapeDtypeStruct(scalars.shape, jnp.float32),
        ),
        in_specs=[vmem, vmem],
        out_specs=(vmem, vmem),
        scratch_shapes=[
            pltpu.VMEM((n,) + flat.shape, jnp.bfloat16),
            pltpu.VMEM((n,) + scalars.shape, jnp.float32),
        ]
        + [pltpu.SemaphoreType.DMA((n,))] * 4,
        compiler_params=pltpu.CompilerParams(collective_id=0, has_side_effects=True),
    )(flat, scalars)
    return out_memory.reshape(memory.shape), out_scalars[:heads, 0]


def block_step(carried, inputs):
    memory, stabilizer = carried
    query_blk, key_blk, value_blk, input_blk, forget_blk = inputs
    length = query_blk.shape[1]
    within = jnp.cumsum(forget_blk, axis=-1)
    causal = jnp.arange(length)[:, None] >= jnp.arange(length)[None, :]
    log_weight = jnp.where(
        causal, within[:, :, None] - within[:, None, :] + input_blk[:, None, :], very_low
    )
    from_state = within + stabilizer[:, None]
    largest = jnp.maximum(from_state, jnp.max(log_weight, axis=-1))
    intra_weight = jnp.exp(log_weight - largest[:, :, None])
    state_weight = jnp.exp(from_state - largest)
    scores = jnp.einsum("htd,hsd->hts", query_blk, key_blk, precision=highest) * intra_weight
    numerator = jnp.einsum("hts,hsv->htv", scores, value_blk, precision=highest) + state_weight[
        :, :, None
    ] * jnp.einsum("htd,hdv->htv", query_blk, memory, precision=highest)
    block_total = within[:, -1]
    to_end = block_total[:, None] - within + input_blk
    new_stabilizer = jnp.maximum(block_total + stabilizer, jnp.max(to_end, axis=-1))
    retain = jnp.exp(block_total + stabilizer - new_stabilizer)
    state_add = jnp.exp(to_end - new_stabilizer[:, None])
    memory = retain[:, None, None] * memory + jnp.einsum(
        "hsd,hsv->hdv", key_blk * state_add[:, :, None], value_blk, precision=highest
    )
    return ((memory, new_stabilizer), (numerator, largest))


def shards(
    queries,
    keys,
    values,
    input_gate_log,
    forget_gate_logits,
    extra_decay_log,
    output_gate_logits,
    head_norm_scale,
    layer_residual_input,
    output_projection_weight,
    expert_norm_scale,
    routing_expert_index,
    routing_expert_weight,
    expert_gate_weight,
    expert_up_weight,
    expert_down_weight,
):
    positions = queries.shape[0]
    heads_here = input_gate_log.shape[0]
    key_width = queries.shape[1] // heads_here
    value_width = values.shape[1] // heads_here
    blocks = positions // BLOCK

    def to_blocks(matrix, columns):
        return (
            matrix.astype(jnp.float32)
            .reshape(blocks, BLOCK, heads_here, columns)
            .transpose(0, 2, 1, 3)
        )

    def gate_blocks(matrix):
        return matrix.reshape(heads_here, blocks, BLOCK).transpose(1, 0, 2)

    query_blocks = to_blocks(queries, key_width) * key_width ** (-0.5)
    key_blocks = to_blocks(keys, key_width)
    value_blocks = to_blocks(values, value_width)
    forget_log_value = jax.nn.log_sigmoid(forget_gate_logits) + extra_decay_log
    sequence_inputs = (
        query_blocks,
        key_blocks,
        value_blocks,
        gate_blocks(input_gate_log),
        gate_blocks(forget_log_value),
    )
    device_decay = jnp.sum(forget_log_value, axis=-1)
    through_here = jnp.cumsum(forget_log_value, axis=-1)
    start_state = (
        jnp.zeros((heads_here, key_width, value_width), jnp.float32),
        jnp.full((heads_here,), very_low, jnp.float32),
    )
    local_state, (numerator, largest) = lax.scan(block_step, start_state, sequence_inputs)
    earlier_memory, earlier_max = incoming_state(device_decay, *local_state)
    from_start = gate_blocks(through_here) + earlier_max[None, :, None]
    combined = jnp.maximum(largest, from_start)
    old_part = jnp.exp(largest - combined)
    new_part = jnp.exp(from_start - combined)
    numerator = old_part[..., None] * numerator + new_part[..., None] * jnp.einsum(
        "bhtd,hdv->bhtv", query_blocks, earlier_memory, precision=highest
    )
    cell_out = numerator.transpose(0, 2, 1, 3).reshape(positions, heads_here, value_width)
    scaled = cell_out * lax.rsqrt(jnp.mean(cell_out * cell_out, axis=-1, keepdims=True) + epsilon)
    gated_out = (
        jax.nn.sigmoid(output_gate_logits.astype(jnp.float32)).reshape(
            positions, heads_here, value_width
        )
        * scaled
        * head_norm_scale.reshape(heads_here, value_width)
    )
    mixture = gated_out.reshape(positions, heads_here * value_width).astype(jnp.bfloat16)
    token_mix = lax.all_to_all(mixture, "tp", split_axis=0, concat_axis=1, tiled=True)
    projected = jnp.dot(token_mix, output_projection_weight, preferred_element_type=jnp.float32)
    middle = (layer_residual_input.astype(jnp.float32) + projected).astype(jnp.bfloat16)
    middle_wide = middle.astype(jnp.float32)
    normed = (
        middle_wide
        * lax.rsqrt(jnp.mean(middle_wide * middle_wide, axis=-1, keepdims=True) + epsilon)
        * expert_norm_scale
    ).astype(jnp.bfloat16)
    tok_count = normed.shape[0]
    model_width = normed.shape[1]
    sp_count = lax.axis_size("sp")
    tp_count = lax.axis_size("tp")
    devices = sp_count * tp_count
    local_experts = expert_gate_weight.shape[0]
    experts = local_experts * devices
    slots = max(2, 2 * tok_count * TOP // experts)
    entries = tok_count * TOP
    flat_ids = routing_expert_index.reshape(-1)
    one_hot = (flat_ids[:, None] == jnp.arange(experts, dtype=jnp.int32)[None, :]).astype(
        jnp.bfloat16
    )
    earlier_rows = (jnp.arange(entries)[:, None] > jnp.arange(entries)[None, :]).astype(
        jnp.bfloat16
    )
    seen_before = jnp.dot(earlier_rows, one_hot, preferred_element_type=jnp.float32)
    position_in = jnp.sum(seen_before * one_hot.astype(jnp.float32), axis=1).astype(jnp.int32)
    slot_key = flat_ids * slots + position_in
    matches = slot_key[None, :] == jnp.arange(experts * slots, dtype=jnp.int32)[:, None]
    pick = jnp.sum(
        matches.reshape(experts * slots, tok_count, TOP).astype(jnp.float32), axis=2
    ).astype(jnp.bfloat16)
    outgoing = (
        jnp.dot(pick, normed, preferred_element_type=jnp.float32)
        .astype(jnp.bfloat16)
        .reshape(experts, slots, model_width)
    )
    arrived = lax.all_to_all(outgoing, ("sp", "tp"), split_axis=0, concat_axis=0, tiled=True)
    grouped = arrived.reshape(devices, local_experts, arrived.shape[1], model_width)
    gate_part = jnp.einsum(
        "sxcd,xdf->sxcf", grouped, expert_gate_weight, preferred_element_type=jnp.float32
    )
    up_part = jnp.einsum(
        "sxcd,xdf->sxcf", grouped, expert_up_weight, preferred_element_type=jnp.float32
    )
    activation = (jax.nn.silu(gate_part) * up_part).astype(jnp.bfloat16)
    produced = jnp.einsum(
        "sxcf,xfd->sxcd", activation, expert_down_weight, preferred_element_type=jnp.float32
    ).astype(jnp.bfloat16)
    returned = lax.all_to_all(
        produced.reshape(arrived.shape), ("sp", "tp"), split_axis=0, concat_axis=0, tiled=True
    )
    returned = returned.reshape(experts * slots, model_width)
    weight_high = lax.reduce_precision(routing_expert_weight, 8, 7)
    slot_pairs = slot_key.reshape(tok_count, TOP, 1)
    slot_range = jnp.arange(experts * slots, dtype=jnp.int32)

    def spread(weights):
        return jnp.sum(
            jnp.where(slot_pairs == slot_range, weights[:, :, None], 0.0), axis=1
        ).astype(jnp.bfloat16)

    expert_sum = jnp.dot(
        spread(weight_high), returned, preferred_element_type=jnp.float32
    ) + jnp.dot(
        spread(routing_expert_weight - weight_high), returned, preferred_element_type=jnp.float32
    )
    return (middle_wide + expert_sum).astype(jnp.bfloat16)


def solution(mesh):
    in_specs = (
        P("sp", "tp"),
        P("sp", "tp"),
        P("sp", "tp"),
        P("tp", "sp"),
        P("tp", "sp"),
        P("tp", "sp"),
        P("sp", "tp"),
        P("tp"),
        P(("sp", "tp"), None),
        P(),
        P(),
        P(("sp", "tp"), None),
        P(("sp", "tp"), None),
        P(("sp", "tp"), None, None),
        P(("sp", "tp"), None, None),
        P(("sp", "tp"), None, None),
    )
    out_specs = P(("sp", "tp"), None)
    return jax.shard_map(shards, mesh=mesh, in_specs=in_specs, out_specs=out_specs, check_vma=False)
```

```python
import functools

import jax
import jax.numpy as jnp
from jax import lax
from jax.experimental import pallas as pl
from jax.experimental.pallas import tpu as pltpu
from jax.sharding import PartitionSpec as P

TOP = 2
BLOCK = 128


very_low = -1e30
epsilon = 1e-06
highest = lax.Precision.HIGHEST
MESH = pl.DeviceIdType.MESH


def join_kernel(n, heads, key_width, memory_ref, scalars_ref, out_memory, out_scalars,
                got_memory, got_scalars, send_memory, send_scalars, recv_memory, recv_scalars):
    me = lax.axis_index("sp")
    barrier = pltpu.get_barrier_semaphore()
    for k in range(1, n):
        other = lax.rem(me + k, n)
        pl.semaphore_signal(barrier, inc=1, device_id={"sp": other}, device_id_type=MESH)
    pl.semaphore_wait(barrier, n - 1)

    def copies(source, target):
        kind = dict(device_id={"sp": target}, device_id_type=MESH)
        return (
            pltpu.make_async_remote_copy(
                src_ref=memory_ref, dst_ref=got_memory.at[source],
                send_sem=send_memory.at[target], recv_sem=recv_memory.at[source], **kind),
            pltpu.make_async_remote_copy(
                src_ref=scalars_ref, dst_ref=got_scalars.at[source],
                send_sem=send_scalars.at[target], recv_sem=recv_scalars.at[source], **kind),
        )

    for k in range(n - 1, 0, -1):
        @pl.when(me + k < n)
        def _(k=k):
            for copy in copies(me, me + k):
                copy.start()

    out_memory[...] = jnp.zeros_like(out_memory)
    out_scalars[...] = jnp.full_like(out_scalars, very_low)

    def lap(j, carry):
        for copy in copies(j, me):
            copy.wait_recv()
        for h in range(heads):
            decay = got_scalars[j, h : h + 1, :]
            stab_late = got_scalars[j, heads + h : heads + h + 1, :]
            shifted = decay + out_scalars[h : h + 1, :]
            combined = jnp.maximum(shifted, stab_late)
            rows = slice(h * key_width, (h + 1) * key_width)
            out_memory[rows, :] = jnp.exp(shifted - combined) * out_memory[rows, :] + jnp.exp(
                stab_late - combined
            ) * got_memory[j, rows, :].astype(jnp.float32)
            out_scalars[h : h + 1, :] = combined
        return carry

    lax.fori_loop(0, me, lap, 0)
    for k in range(1, n):
        @pl.when(me + k < n)
        def _(k=k):
            for copy in copies(me, me + k):
                copy.wait_send()


def incoming_state(decay, memory, stabilizer):
    heads, key_width, value_width = memory.shape
    n = lax.axis_size("sp")
    scalar_rows = -(-2 * heads // 8) * 8
    scalars = jnp.concatenate(
        [decay, stabilizer, jnp.zeros((scalar_rows - 2 * heads,), jnp.float32)]
    )
    scalars = jnp.broadcast_to(scalars[:, None], (scalar_rows, value_width))
    flat = memory.reshape(heads * key_width, value_width).astype(jnp.bfloat16)
    vmem = pl.BlockSpec(memory_space=pltpu.VMEM)
    out_memory, out_scalars = pl.pallas_call(
        functools.partial(join_kernel, n, heads, key_width),
        out_shape=(
            jax.ShapeDtypeStruct(flat.shape, jnp.float32),
            jax.ShapeDtypeStruct(scalars.shape, jnp.float32),
        ),
        in_specs=[vmem, vmem],
        out_specs=(vmem, vmem),
        scratch_shapes=[
            pltpu.VMEM((n,) + flat.shape, jnp.bfloat16),
            pltpu.VMEM((n,) + scalars.shape, jnp.float32),
        ]
        + [pltpu.SemaphoreType.DMA((n,))] * 4,
        compiler_params=pltpu.CompilerParams(collective_id=0, has_side_effects=True),
    )(flat, scalars)
    return out_memory.reshape(memory.shape), out_scalars[:heads, 0]


def all_blocks(query_blk, key_blk, value_blk, input_blk, forget_blk):
    blocks, heads, length = forget_blk.shape
    within = jnp.cumsum(forget_blk, axis=-1)
    causal = jnp.arange(length)[:, None] >= jnp.arange(length)[None, :]
    log_weight = jnp.where(
        causal, within[..., :, None] - within[..., None, :] + input_blk[..., None, :], very_low
    )
    largest = jnp.max(log_weight, axis=-1)
    intra_weight = jnp.exp(log_weight - largest[..., None])
    scores = jnp.einsum("bhtd,bhsd->bhts", query_blk, key_blk, precision=highest) * intra_weight
    numerator = jnp.einsum("bhts,bhsv->bhtv", scores, value_blk, precision=highest)
    block_total = within[..., -1]
    to_end = block_total[..., None] - within + input_blk
    block_max = jnp.max(to_end, axis=-1)
    state_add = jnp.exp(to_end - block_max[..., None])
    block_memory = jnp.einsum(
        "bhsd,bhsv->bhdv", key_blk * state_add[..., None], value_blk, precision=highest
    )
    before = [jnp.zeros((heads,), jnp.float32)]
    memories = [jnp.zeros(block_memory.shape[1:], jnp.float32)]
    maxima = [jnp.full((heads,), very_low, jnp.float32)]
    for b in range(blocks):
        shifted = maxima[b] + block_total[b]
        combined = jnp.maximum(shifted, block_max[b])
        memories.append(
            jnp.exp(shifted - combined)[:, None, None] * memories[b]
            + jnp.exp(block_max[b] - combined)[:, None, None] * block_memory[b]
        )
        maxima.append(combined)
        before.append(before[b] + block_total[b])
    return (numerator, largest, within), (before, memories, maxima)


def expert_kernel(peers, count, members, tile,
                  sent_ref, gate_ref, up_ref, down_ref, high_ref, low_ref, middle_ref, out_ref,
                  arrived, produced, returned, activation, gate_w, up_w, down_w,
                  send_there, recv_there, send_back, recv_back, weight_sems):
    sp = lax.axis_index("sp")
    me = sp * peers + lax.axis_index("tp")
    groups = count // members
    own_group = me // members
    slots, width = sent_ref.shape[1:]
    hidden = gate_w.shape[1]

    def place(device):
        return dict(
            device_id={"sp": device // peers, "tp": lax.rem(device, peers)}, device_id_type=MESH
        )

    weight_copies = [
        pltpu.make_async_copy(source.at[0], target, weight_sems.at[k])
        for k, (source, target) in enumerate(
            ((gate_ref, gate_w), (up_ref, up_w), (down_ref, down_w))
        )
    ]
    for copy in weight_copies:
        copy.start()

    def there(source, target):
        return pltpu.make_async_remote_copy(
            src_ref=sent_ref.at[target], dst_ref=arrived.at[source],
            send_sem=send_there.at[target], recv_sem=recv_there.at[source], **place(target))

    def back(source, target):
        return pltpu.make_async_remote_copy(
            src_ref=produced.at[target], dst_ref=returned.at[source],
            send_sem=send_back.at[target], recv_sem=recv_back.at[source], **place(target))

    barrier = pltpu.get_barrier_semaphore()

    def greet(k, carry):
        pl.semaphore_signal(barrier, inc=1, **place(lax.rem(me + k, count)))
        return carry

    lax.fori_loop(1, count, greet, 0)
    pl.semaphore_wait(barrier, count - 1)

    def group_of(step):
        return lax.rem(own_group + lax.rem(step, 2) * (groups // 2) + step // 2, groups)

    def dispatch(index, carry):
        target = group_of(lax.rem(index // members + 1, groups)) * members + lax.rem(index, members)

        @pl.when(target != me)
        def _():
            there(me, target).start()

        return carry

    lax.fori_loop(0, count, dispatch, 0)
    arrived[me] = sent_ref[me]
    for copy in weight_copies:
        copy.wait()

    def one_group(step, carry):
        first = group_of(step) * members

        def receive(j, carry):
            @pl.when(first + j != me)
            def _():
                there(first + j, me).wait_recv()

            return carry

        lax.fori_loop(0, members, receive, 0)

        def hidden_tile(t, carry):
            columns = pl.ds(pl.multiple_of(t * tile, tile), tile)
            rows = arrived[pl.ds(first, members)].reshape(members * slots, width)
            gate_part = jnp.dot(rows, gate_w[:, columns], preferred_element_type=jnp.float32)
            up_part = jnp.dot(rows, up_w[:, columns], preferred_element_type=jnp.float32)
            activation[:, columns] = (jax.nn.silu(gate_part) * up_part).astype(jnp.bfloat16)
            return carry

        lax.fori_loop(0, hidden // tile, hidden_tile, 0)

        def width_tile(t, carry):
            columns = pl.ds(pl.multiple_of(t * tile, tile), tile)
            part = jnp.dot(
                activation[...], down_w[:, columns], preferred_element_type=jnp.float32
            ).astype(jnp.bfloat16)
            produced[pl.ds(first, members), :, columns] = part.reshape(members, slots, tile)
            return carry

        lax.fori_loop(0, width // tile, width_tile, 0)

        def give_back(j, carry):
            @pl.when(first + j != me)
            def _():
                back(me, first + j).start()

            return carry

        lax.fori_loop(0, members, give_back, 0)
        return carry

    lax.fori_loop(0, groups, one_group, 0)
    returned[me] = produced[me]

    def collect(k, carry):
        back(lax.rem(me + k, count), me).wait_recv()
        return carry

    lax.fori_loop(1, count, collect, 0)

    def combine_tile(t, carry):
        columns = pl.ds(pl.multiple_of(t * tile, tile), tile)
        rows = returned[:, :, columns].reshape(count * slots, tile)
        total = jnp.dot(high_ref[...], rows, preferred_element_type=jnp.float32) + jnp.dot(
            low_ref[...], rows, preferred_element_type=jnp.float32
        )
        out_ref[:, columns] = (middle_ref[:, columns].astype(jnp.float32) + total).astype(
            jnp.bfloat16
        )
        return carry

    lax.fori_loop(0, width // tile, combine_tile, 0)

    def finish(k, carry):
        target = lax.rem(me + k, count)
        there(me, target).wait_send()
        back(me, target).wait_send()
        return carry

    lax.fori_loop(1, count, finish, 0)


def expert_call(sent, gate, up, down, high, low, middle):
    count, slots, width = sent.shape
    hidden = gate.shape[2]
    peers = lax.axis_size("tp")
    vmem = pl.BlockSpec(memory_space=pltpu.VMEM)
    anywhere = pl.BlockSpec(memory_space=pl.ANY)
    members = count // 4
    return pl.pallas_call(
        functools.partial(expert_kernel, peers, count, members, 256),
        out_shape=jax.ShapeDtypeStruct(middle.shape, jnp.bfloat16),
        in_specs=[vmem, anywhere, anywhere, anywhere, vmem, vmem, vmem],
        out_specs=vmem,
        scratch_shapes=[
            pltpu.VMEM(sent.shape, jnp.bfloat16),
            pltpu.VMEM(sent.shape, jnp.bfloat16),
            pltpu.VMEM(sent.shape, jnp.bfloat16),
            pltpu.VMEM((members * slots, hidden), jnp.bfloat16),
            pltpu.VMEM((width, hidden), jnp.bfloat16),
            pltpu.VMEM((width, hidden), jnp.bfloat16),
            pltpu.VMEM((hidden, width), jnp.bfloat16),
        ]
        + [pltpu.SemaphoreType.DMA((count,))] * 4
        + [pltpu.SemaphoreType.DMA((3,))],
        compiler_params=pltpu.CompilerParams(collective_id=1, has_side_effects=True),
    )(sent, gate, up, down, high, low, middle)


def shards(
    queries,
    keys,
    values,
    input_gate_log,
    forget_gate_logits,
    extra_decay_log,
    output_gate_logits,
    head_norm_scale,
    layer_residual_input,
    output_projection_weight,
    expert_norm_scale,
    routing_expert_index,
    routing_expert_weight,
    expert_gate_weight,
    expert_up_weight,
    expert_down_weight,
):
    positions = queries.shape[0]
    heads_here = input_gate_log.shape[0]
    key_width = queries.shape[1] // heads_here
    value_width = values.shape[1] // heads_here
    blocks = positions // BLOCK

    def to_blocks(matrix, columns):
        return (
            matrix.astype(jnp.float32)
            .reshape(blocks, BLOCK, heads_here, columns)
            .transpose(0, 2, 1, 3)
        )

    def gate_blocks(matrix):
        return matrix.reshape(heads_here, blocks, BLOCK).transpose(1, 0, 2)

    query_blocks = to_blocks(queries, key_width) * key_width ** (-0.5)
    key_blocks = to_blocks(keys, key_width)
    value_blocks = to_blocks(values, value_width)
    forget_log_value = jax.nn.log_sigmoid(forget_gate_logits) + extra_decay_log
    sequence_inputs = (
        query_blocks,
        key_blocks,
        value_blocks,
        gate_blocks(input_gate_log),
        gate_blocks(forget_log_value),
    )
    (numerator, largest, within), (before, memories, maxima) = all_blocks(*sequence_inputs)
    earlier_memory, earlier_max = incoming_state(before[-1], memories[-1], maxima[-1])
    local_max = jnp.stack(maxima[:-1])
    moved_max = jnp.stack(before[:-1]) + earlier_max[None, :]
    start_max = jnp.maximum(moved_max, local_max)
    start_memory = (
        jnp.exp(moved_max - start_max)[..., None, None] * earlier_memory[None]
        + jnp.exp(local_max - start_max)[..., None, None] * jnp.stack(memories[:-1])
    )
    from_start = within + start_max[..., None]
    combined = jnp.maximum(largest, from_start)
    old_part = jnp.exp(largest - combined)
    new_part = jnp.exp(from_start - combined)
    numerator = old_part[..., None] * numerator + new_part[..., None] * jnp.einsum(
        "bhtd,bhdv->bhtv", query_blocks, start_memory, precision=highest
    )
    cell_out = numerator.transpose(0, 2, 1, 3).reshape(positions, heads_here, value_width)
    scaled = cell_out * lax.rsqrt(jnp.mean(cell_out * cell_out, axis=-1, keepdims=True) + epsilon)
    gated_out = (
        jax.nn.sigmoid(output_gate_logits.astype(jnp.float32)).reshape(
            positions, heads_here, value_width
        )
        * scaled
        * head_norm_scale.reshape(heads_here, value_width)
    )
    mixture = gated_out.reshape(positions, heads_here * value_width).astype(jnp.bfloat16)
    token_mix = lax.all_to_all(mixture, "tp", split_axis=0, concat_axis=1, tiled=True)
    projected = jnp.dot(token_mix, output_projection_weight, preferred_element_type=jnp.float32)
    middle = (layer_residual_input.astype(jnp.float32) + projected).astype(jnp.bfloat16)
    middle_wide = middle.astype(jnp.float32)
    normed = (
        middle_wide
        * lax.rsqrt(jnp.mean(middle_wide * middle_wide, axis=-1, keepdims=True) + epsilon)
        * expert_norm_scale
    ).astype(jnp.bfloat16)
    tok_count = normed.shape[0]
    model_width = normed.shape[1]
    sp_count = lax.axis_size("sp")
    tp_count = lax.axis_size("tp")
    devices = sp_count * tp_count
    local_experts = expert_gate_weight.shape[0]
    experts = local_experts * devices
    slots = max(2, 2 * tok_count * TOP // experts)
    entries = tok_count * TOP
    flat_ids = routing_expert_index.reshape(-1)
    one_hot = (flat_ids[:, None] == jnp.arange(experts, dtype=jnp.int32)[None, :]).astype(
        jnp.bfloat16
    )
    earlier_rows = (jnp.arange(entries)[:, None] > jnp.arange(entries)[None, :]).astype(
        jnp.bfloat16
    )
    seen_before = jnp.dot(earlier_rows, one_hot, preferred_element_type=jnp.float32)
    position_in = jnp.sum(seen_before * one_hot.astype(jnp.float32), axis=1).astype(jnp.int32)
    slot_key = flat_ids * slots + position_in
    matches = slot_key[None, :] == jnp.arange(experts * slots, dtype=jnp.int32)[:, None]
    pick = jnp.sum(
        matches.reshape(experts * slots, tok_count, TOP).astype(jnp.float32), axis=2
    ).astype(jnp.bfloat16)
    outgoing = (
        jnp.dot(pick, normed, preferred_element_type=jnp.float32)
        .astype(jnp.bfloat16)
        .reshape(experts, slots, model_width)
    )
    weight_high = lax.reduce_precision(routing_expert_weight, 8, 7)
    slot_pairs = slot_key.reshape(tok_count, TOP, 1)
    slot_range = jnp.arange(experts * slots, dtype=jnp.int32)

    def spread(weights):
        return jnp.sum(
            jnp.where(slot_pairs == slot_range, weights[:, :, None], 0.0), axis=1
        ).astype(jnp.bfloat16)

    high = spread(weight_high)
    low = spread(routing_expert_weight - weight_high)
    if local_experts == 1 and slots % 16 == 0 and devices % 4 == 0:
        return expert_call(
            outgoing, expert_gate_weight, expert_up_weight, expert_down_weight, high, low, middle
        )
    arrived = lax.all_to_all(outgoing, ("sp", "tp"), split_axis=0, concat_axis=0, tiled=True)
    grouped = arrived.reshape(devices, local_experts, arrived.shape[1], model_width)
    gate_part = jnp.einsum(
        "sxcd,xdf->sxcf", grouped, expert_gate_weight, preferred_element_type=jnp.float32
    )
    up_part = jnp.einsum(
        "sxcd,xdf->sxcf", grouped, expert_up_weight, preferred_element_type=jnp.float32
    )
    activation = (jax.nn.silu(gate_part) * up_part).astype(jnp.bfloat16)
    produced = jnp.einsum(
        "sxcf,xfd->sxcd", activation, expert_down_weight, preferred_element_type=jnp.float32
    ).astype(jnp.bfloat16)
    returned = lax.all_to_all(
        produced.reshape(arrived.shape), ("sp", "tp"), split_axis=0, concat_axis=0, tiled=True
    )
    returned = returned.reshape(experts * slots, model_width)
    expert_sum = jnp.dot(high, returned, preferred_element_type=jnp.float32) + jnp.dot(
        low, returned, preferred_element_type=jnp.float32
    )
    return (middle_wide + expert_sum).astype(jnp.bfloat16)


def solution(mesh):
    in_specs = (
        P("sp", "tp"),
        P("sp", "tp"),
        P("sp", "tp"),
        P("tp", "sp"),
        P("tp", "sp"),
        P("tp", "sp"),
        P("sp", "tp"),
        P("tp"),
        P(("sp", "tp"), None),
        P(),
        P(),
        P(("sp", "tp"), None),
        P(("sp", "tp"), None),
        P(("sp", "tp"), None, None),
        P(("sp", "tp"), None, None),
        P(("sp", "tp"), None, None),
    )
    out_specs = P(("sp", "tp"), None)
    return jax.shard_map(shards, mesh=mesh, in_specs=in_specs, out_specs=out_specs, check_vma=False)
```
